32 devices in a mesh: fs: 8 (over z, x), tp: 4 (over y, core).
Axes of the slice: x: 2, y: 2, z: 4, core: 2. Of those that a mesh axis runs over, the one named last changes fastest.
Arguments:
- saved_input: bfloat16 [20480, 2048], P('fs'), may hold values from -6 to 6
- value_cot: bfloat16 [20480, 1024], P('fs', 'tp'), may hold values from -6 to 6
- query_cot: bfloat16 [20480, 512], P('fs', 'tp'), may hold values from -6 to 6
- value_master: float32 [2048, 1024], P('fs', 'tp'), may hold values from -0.125 to 0.125
- query_master: float32 [2048, 512], P('fs', 'tp'), may hold values from -0.125 to 0.125
- value_factor: bfloat16 [2048, 256], P('fs'), may hold values from -0.125 to 0.125
- query_factor: bfloat16 [2048, 256], P('fs'), may hold values from -0.125 to 0.125
- value_first: float32 [256, 1024], P('fs', 'tp'), as said below
- value_second: float32 [256, 1024], P('fs', 'tp'), as said below
- query_first: float32 [256, 512], P('fs', 'tp'), as said below
- query_second: float32 [256, 512], P('fs', 'tp'), as said below
Outputs:
- value_step: float32 [2048, 1024], P('fs', 'tp')
- query_step: float32 [2048, 512], P('fs', 'tp')
- value_master_new: float32 [2048, 1024], P('fs', 'tp')
- query_master_new: float32 [2048, 512], P('fs', 'tp')
- value_copy: bfloat16 [2048, 1024], P(None, 'tp')
- query_copy: bfloat16 [2048, 512], P(None, 'tp')
- value_first_new: float32 [256, 1024], P('fs', 'tp')
- value_second_new: float32 [256, 1024], P('fs', 'tp')
- query_first_new: float32 [256, 512], P('fs', 'tp')
- query_second_new: float32 [256, 512], P('fs', 'tp')
The draws below stay inside these ranges and needn't reach their ends.
Inputs may be any that keep to these rules, and one draw needn't show every extreme that they name: `value_first`: first moments are real-valued of the projected gradient's order. `value_second`: second moments are positive. `query_first`: first moments are real-valued of the projected gradient's order. `query_second`: second moments are positive.
All inputs are finite; a program needn't handle non-finite values.
Results may differ from the reference program's by a relative error of at most 0.001.
Values may be sent and summed in bfloat16 or wider, within the bound.
No kernel may reach another device: no remote copies, remote signals or barrier semaphores. Data moves between devices by JAX's collectives and lax.ppermute only.
A program may use at most 64 MiB of HBM per device.

```python
import jax
import jax.numpy as jnp
from jax import lax

D = 2048
RANK = 256
TOKENS = 20480
V_W = 1024
QK_W = 512


def first_draw(key, width):
    level = 0.1 / jnp.sqrt(jnp.float32(TOKENS))
    values = jax.random.normal(jax.random.fold_in(key, 11), (RANK, width), jnp.float32)
    return values * level


def second_draw(key, width):
    level = 0.05 / jnp.float32(TOKENS)
    row_pos = jnp.arange(RANK, dtype=jnp.float32)[:, None] / RANK
    col_pos = jnp.arange(width, dtype=jnp.float32)[None, :] / width
    spread = jnp.exp(jax.random.uniform(jax.random.fold_in(key, 13), (RANK, width), jnp.float32, -0.7, 0.7))
    rising = 10.0 ** row_pos * 10.0 ** col_pos
    return level * spread * rising


def draw_value_first(key, part):
    return first_draw(key, V_W)


def draw_value_second(key, part):
    return second_draw(key, V_W)


def draw_query_first(key, part):
    return first_draw(key, QK_W)


def draw_query_second(key, part):
    return second_draw(key, QK_W)


def strengthened(entries, own_key, source, target, shards_of, factor):
    owner, partner = [(jnp.arange(entries.shape[axis_at]) // (entries.shape[axis_at] // shards_of)).reshape([-1 if axis == axis_at else 1 for axis in range(entries.ndim)]) for axis_at in (source, target)]
    chosen = jax.random.permutation(own_key, shards_of)[partner]
    strong = (owner == chosen) | (owner == (partner + shards_of // 2) % shards_of)
    return jnp.where(strong, factor * entries, entries)


def steps_of(stream_key, dims, pieces, smallest, top_value):
    factor_of, own = 1.0, jax.random.fold_in(stream_key, 6)
    for position, shards_of in pieces:
        draws = jnp.exp(jax.random.uniform(jax.random.fold_in(own, position), (shards_of,), jnp.float32, smallest / len(pieces), top_value / len(pieces)))
        factor_of = factor_of * jnp.repeat(draws, dims[position] // shards_of).reshape([-1 if axis == position else 1 for axis in range(len(dims))])
    return factor_of


def noise(key, dims, scale, bound, cuts=(), held_as=jnp.bfloat16):
    values = scale * jax.random.normal(key, dims, jnp.float32)
    if cuts:
        values = values * steps_of(key, dims, cuts, -0.22, 0.18)
    return jnp.clip(values, -bound, bound).astype(held_as)


def heavy_noise(rng, dims, scale, bound, shards, heavy, kind=jnp.bfloat16):
    values = scale * jax.random.normal(rng, dims, jnp.float32)
    if shards:
        values = values * steps_of(rng, dims, shards, -0.22, 0.18)
    return jnp.clip(strengthened(values, jax.random.fold_in(rng, 3), *heavy), -bound, bound).astype(kind)


def setup_inputs(seed: int = 0) -> dict:
    arg_keys = jax.random.split(jax.random.key(seed), 12)
    return {
        "saved_input": heavy_noise(arg_keys[0], (TOKENS, D), 1.0, 6.0, ((0, 8),), (0, 1, 8, 2.0)),
        "value_cot": noise(arg_keys[1], (TOKENS, V_W), 1.0, 6.0, ((0, 8), (1, 4))),
        "query_cot": noise(arg_keys[2], (TOKENS, QK_W), 1.0, 6.0, ((0, 8), (1, 4))),
        "value_master": noise(arg_keys[3], (D, V_W), D ** -0.5, 0.125, ((0, 8), (1, 4)), jnp.float32),
        "query_master": noise(arg_keys[4], (D, QK_W), D ** -0.5, 0.125, ((0, 8), (1, 4)), jnp.float32),
        "value_factor": noise(arg_keys[5], (D, RANK), D ** -0.5, 0.125, ((0, 8),)),
        "query_factor": noise(arg_keys[6], (D, RANK), D ** -0.5, 0.125, ((0, 8),)),
        "value_first": draw_value_first(jax.random.fold_in(arg_keys[11], 71), 0),
        "value_second": draw_value_second(jax.random.fold_in(arg_keys[11], 71), 0),
        "query_first": draw_query_first(jax.random.fold_in(arg_keys[11], 71), 0),
        "query_second": draw_query_second(jax.random.fold_in(arg_keys[11], 71), 0),
    }


BETA_ONE = 0.9
BETA_TWO = 0.95
DENOM_EPS = 1e-08
NORM_EPS = 1e-06
STEP_SIZE = 0.05

def moment_update(factor, gradient, first, second):
    projected = jnp.dot(factor.astype(jnp.float32).T, gradient, precision=lax.Precision.HIGHEST)
    first_new = BETA_ONE * first + (1.0 - BETA_ONE) * projected
    second_new = BETA_TWO * second + (1.0 - BETA_TWO) * projected * projected
    direction = first_new / (jnp.sqrt(second_new) + DENOM_EPS)
    return (first_new, second_new, direction)

def reference(saved_input, value_cot, query_cot, value_master, query_master, value_factor, query_factor, value_first, value_second, query_first, query_second):
    value_grad = jnp.dot(saved_input.T, value_cot, preferred_element_type=jnp.float32) / TOKENS
    query_grad = jnp.dot(saved_input.T, query_cot, preferred_element_type=jnp.float32) / TOKENS
    value_first_new, value_second_new, value_direction = moment_update(value_factor, value_grad, value_first, value_second)
    query_first_new, query_second_new, query_direction = moment_update(query_factor, query_grad, query_first, query_second)
    square_sum = jnp.sum(value_direction * value_direction) + jnp.sum(query_direction * query_direction)
    update_scale = 1.0 / jnp.sqrt(square_sum / (RANK * (V_W + QK_W)) + NORM_EPS)
    value_step = jnp.dot(value_factor.astype(jnp.float32), value_direction, precision=lax.Precision.HIGHEST) * update_scale
    query_step = jnp.dot(query_factor.astype(jnp.float32), query_direction, precision=lax.Precision.HIGHEST) * update_scale
    value_master_new = value_master - STEP_SIZE * value_step
    query_master_new = query_master - STEP_SIZE * query_step
    return (value_step, query_step, value_master_new, query_master_new, value_master_new.astype(jnp.bfloat16), query_master_new.astype(jnp.bfloat16), value_first_new, value_second_new, query_first_new, query_second_new)
```

```python
import jax
import jax.numpy as jnp
from jax import lax
from jax.sharding import PartitionSpec as P

BETA_ONE = 0.9
BETA_TWO = 0.95
DENOM_EPS = 1e-08
NORM_EPS = 1e-06
STEP_SIZE = 0.05


def moment_update(projected, first, second):
    first_new = BETA_ONE * first + (1.0 - BETA_ONE) * projected
    second_new = BETA_TWO * second + (1.0 - BETA_TWO) * projected * projected
    direction = first_new / (jnp.sqrt(second_new) + DENOM_EPS)
    return (first_new, second_new, direction)


def in_two(values):
    head = lax.reduce_precision(values, 8, 7)
    return head.astype(jnp.bfloat16), (values - head).astype(jnp.bfloat16)


def dot_in_two(left, right, contract):
    dims = ((contract, (0,)), ((), ()))
    return sum(
        lax.dot_general(left, piece, dims, preferred_element_type=jnp.float32)
        for piece in in_two(right)
    )


def partner(value, axis, step):
    count = lax.axis_size(axis)
    return lax.ppermute(value, axis, [(i, partner_of(i, step, count)) for i in range(count)])


def partner_of(index, step, count):
    return index ^ step if count & (count - 1) == 0 else (index + step) % count


def source_of(index, step, count):
    return index ^ step if count & (count - 1) == 0 else (index - step) % count


def gather_by_permutes(own):
    count, index = lax.axis_size("fs"), lax.axis_index("fs")
    pieces = [own] + [partner(own, "fs", step) for step in range(1, count)]
    rows = own.shape[0]
    whole = jnp.zeros((count * rows,) + own.shape[1:], own.dtype)
    for step, piece in enumerate(pieces):
        at = source_of(index, step, count) * rows
        whole = lax.dynamic_update_slice(whole, piece, (at, 0))
    return whole


def gather_by_exchange(own):
    count = lax.axis_size("fs")
    sent = jnp.broadcast_to(own[None], (count,) + own.shape)
    got = lax.all_to_all(sent, "fs", 0, 0, tiled=True)
    return got.reshape((count * own.shape[0],) + own.shape[1:])


def on_device(
    saved_input,
    value_cot,
    query_cot,
    value_master,
    query_master,
    value_factor,
    query_factor,
    value_first,
    value_second,
    query_first,
    query_second,
):
    shards = lax.axis_size("fs")
    groups = lax.axis_size("tp")
    width = value_cot.shape[1]
    tokens_all = saved_input.shape[0] * shards
    even = lax.axis_index("tp") % 2 == 0
    mine = gather_by_permutes(jnp.where(even, value_factor, query_factor))
    other = lax.ppermute(mine, "tp", [(i, i ^ 1) for i in range(groups)])
    gradient = (
        lax.dot_general(
            saved_input,
            jnp.concatenate([value_cot, query_cot], axis=1),
            (((0,), (0,)), ((), ())),
            preferred_element_type=jnp.float32,
        )
        / tokens_all
    )
    by_mine = dot_in_two(mine, gradient, (0,))
    by_other = dot_in_two(other, gradient, (0,))
    part = jnp.concatenate(
        [
            jnp.where(even, by_mine[:, :width], by_other[:, :width]),
            jnp.where(even, by_other[:, width:], by_mine[:, width:]),
        ],
        axis=1,
    )
    own_rows = part.shape[0] // shards
    share = lax.all_to_all(part.reshape(shards, own_rows, -1), "fs", 0, 0, tiled=True).sum(0)
    value_first_new, value_second_new, value_dir_own = moment_update(
        share[:, :width], value_first, value_second
    )
    query_first_new, query_second_new, query_dir_own = moment_update(
        share[:, width:], query_first, query_second
    )
    direction = gather_by_permutes(jnp.concatenate([value_dir_own, query_dir_own], axis=1))
    square_sum = jnp.sum(direction * direction).reshape(1, 1)
    square_sum = square_sum + sum(
        partner(square_sum, "tp", step) for step in range(1, groups)
    )
    update_scale = 1.0 / jnp.sqrt(square_sum / (direction.shape[0] * (direction.shape[1] * groups)) + NORM_EPS)
    value_step = dot_in_two(value_factor, direction[:, :width], (1,)) * update_scale
    query_step = dot_in_two(query_factor, direction[:, width:], (1,)) * update_scale
    value_master_new = value_master - STEP_SIZE * value_step
    query_master_new = query_master - STEP_SIZE * query_step
    both = gather_by_permutes(
        jnp.concatenate([value_master_new, query_master_new], axis=1).astype(jnp.bfloat16)
    )
    value_copy, query_copy = both[:, :width], both[:, width:]
    return (
        value_step,
        query_step,
        value_master_new,
        query_master_new,
        value_copy,
        query_copy,
        value_first_new,
        value_second_new,
        query_first_new,
        query_second_new,
    )


def solution(mesh):
    in_specs = (
        P("fs", None),
        P("fs", "tp"),
        P("fs", "tp"),
        P("fs", "tp"),
        P("fs", "tp"),
        P("fs", None),
        P("fs", None),
        P("fs", "tp"),
        P("fs", "tp"),
        P("fs", "tp"),
        P("fs", "tp"),
    )
    out_specs = (
        P("fs", "tp"),
        P("fs", "tp"),
        P("fs", "tp"),
        P("fs", "tp"),
        P(None, "tp"),
        P(None, "tp"),
        P("fs", "tp"),
        P("fs", "tp"),
        P("fs", "tp"),
        P("fs", "tp"),
    )
    return jax.shard_map(
        on_device, mesh=mesh, in_specs=in_specs, out_specs=out_specs, check_vma=False
    )
```

```python
import jax
import jax.numpy as jnp
from jax import lax
from jax.sharding import PartitionSpec as P

BETA_ONE = 0.9
BETA_TWO = 0.95
DENOM_EPS = 1e-08
NORM_EPS = 1e-06
STEP_SIZE = 0.05


def moment_update(projected, first, second):
    first_new = BETA_ONE * first + (1.0 - BETA_ONE) * projected
    second_new = BETA_TWO * second + (1.0 - BETA_TWO) * projected * projected
    direction = first_new / (jnp.sqrt(second_new) + DENOM_EPS)
    return (first_new, second_new, direction)


def in_two(values):
    head = lax.reduce_precision(values, 8, 7)
    return head.astype(jnp.bfloat16), (values - head).astype(jnp.bfloat16)


def dot_in_two(left, right, contract):
    dims = ((contract, (0,)), ((), ()))
    return sum(
        lax.dot_general(left, piece, dims, preferred_element_type=jnp.float32)
        for piece in in_two(right)
    )


def partner(value, axis, step):
    count = lax.axis_size(axis)
    return lax.ppermute(value, axis, [(i, partner_of(i, step, count)) for i in range(count)])


def partner_of(index, step, count):
    return index ^ step if count & (count - 1) == 0 else (index + step) % count


def source_of(index, step, count):
    return index ^ step if count & (count - 1) == 0 else (index - step) % count


def pieces_in_stages(own):
    count = lax.axis_size("fs")
    if count & (count - 1) or count < 4:
        return [own] + [partner(own, "fs", step) for step in range(1, count)]
    pieces = {0: own}
    for step in range(2, count, 2):
        pieces[step] = partner(own, "fs", step)
    for step in range(0, count, 2):
        pieces[step + 1] = partner(pieces[step], "fs", 1)
    return [pieces[step] for step in range(count)]


def direct_pieces(own):
    return [own] + [partner(own, "fs", step) for step in range(1, lax.axis_size("fs"))]


def placed(pieces):
    count, index = lax.axis_size("fs"), lax.axis_index("fs")
    rows = pieces[0].shape[0]
    whole = jnp.zeros((count * rows,) + pieces[0].shape[1:], pieces[0].dtype)
    for step, piece in enumerate(pieces):
        at = source_of(index, step, count) * rows
        whole = lax.dynamic_update_slice(whole, piece, (at, 0))
    return whole


def on_device(
    saved_input,
    value_cot,
    query_cot,
    value_master,
    query_master,
    value_factor,
    query_factor,
    value_first,
    value_second,
    query_first,
    query_second,
):
    shards = lax.axis_size("fs")
    groups = lax.axis_size("tp")
    width = value_cot.shape[1]
    tokens_all = saved_input.shape[0] * shards
    even = lax.axis_index("tp") % 2 == 0
    factor_pieces = pieces_in_stages(jnp.where(even, value_factor, query_factor))
    gradient = (
        lax.dot_general(
            saved_input,
            jnp.concatenate([value_cot, query_cot], axis=1),
            (((0,), (0,)), ((), ())),
            preferred_element_type=jnp.float32,
        )
        / tokens_all
    )
    factor_pieces[-1], gradient = lax.optimization_barrier((factor_pieces[-1], gradient))
    mine = placed(factor_pieces)
    other = lax.ppermute(mine, "tp", [(i, i ^ 1) for i in range(groups)])
    by_mine = dot_in_two(mine, gradient, (0,))
    by_other = dot_in_two(other, gradient, (0,))
    part = jnp.concatenate(
        [
            jnp.where(even, by_mine[:, :width], by_other[:, :width]),
            jnp.where(even, by_other[:, width:], by_mine[:, width:]),
        ],
        axis=1,
    )
    own_rows = part.shape[0] // shards
    share = lax.all_to_all(part.reshape(shards, own_rows, -1), "fs", 0, 0, tiled=True).sum(0)
    value_first_new, value_second_new, value_dir_own = moment_update(
        share[:, :width], value_first, value_second
    )
    query_first_new, query_second_new, query_dir_own = moment_update(
        share[:, width:], query_first, query_second
    )
    direction = placed(pieces_in_stages(jnp.concatenate([value_dir_own, query_dir_own], axis=1)))
    square_sum = jnp.sum(direction * direction).reshape(1, 1)
    square_sum = square_sum + sum(
        partner(square_sum, "tp", step) for step in range(1, groups)
    )
    update_scale = 1.0 / jnp.sqrt(square_sum / (direction.shape[0] * (direction.shape[1] * groups)) + NORM_EPS)
    value_step = dot_in_two(value_factor, direction[:, :width], (1,)) * update_scale
    query_step = dot_in_two(query_factor, direction[:, width:], (1,)) * update_scale
    value_master_new = value_master - STEP_SIZE * value_step
    query_master_new = query_master - STEP_SIZE * query_step
    copies = pieces_in_stages(
        jnp.concatenate([value_master_new, query_master_new], axis=1).astype(jnp.bfloat16)
    )
    value_copy = placed([piece[:, :width] for piece in copies])
    query_copy = placed([piece[:, width:] for piece in copies])
    return (
        value_step,
        query_step,
        value_master_new,
        query_master_new,
        value_copy,
        query_copy,
        value_first_new,
        value_second_new,
        query_first_new,
        query_second_new,
    )


def solution(mesh):
    in_specs = (
        P("fs", None),
        P("fs", "tp"),
        P("fs", "tp"),
        P("fs", "tp"),
        P("fs", "tp"),
        P("fs", None),
        P("fs", None),
        P("fs", "tp"),
        P("fs", "tp"),
        P("fs", "tp"),
        P("fs", "tp"),
    )
    out_specs = (
        P("fs", "tp"),
        P("fs", "tp"),
        P("fs", "tp"),
        P("fs", "tp"),
        P(None, "tp"),
        P(None, "tp"),
        P("fs", "tp"),
        P("fs", "tp"),
        P("fs", "tp"),
        P("fs", "tp"),
    )
    return jax.shard_map(
        on_device, mesh=mesh, in_specs=in_specs, out_specs=out_specs, check_vma=False
    )
```
